32 devices in a mesh: fs: 8 (over z, y), tp: 4 (over x, core).
Axes of the slice: x: 2, y: 2, z: 4, core: 2. Of those that a mesh axis runs over, the one named last changes fastest.
Arguments:
- prompt: bfloat16 [4096, 4096], P('fs'), may hold values from -6 to 6
- expert_ids: int32 [4096, 2], P('fs'), may hold values from 0 to 15, all different within a row; in each aligned block of 512 rows (0 to 511, 512 to 1023, ...) at most 96 rows name the same one
- group_weight: float32 [4096], P('fs'), may hold values from 0.25 to 1
- expert_share: float32 [4096, 2], P('fs'), may hold values from 0.1 to 1
- norm_gain: float32 [4096], P('fs'), may hold values from 0.1 to 1.9
- gate_train: float32 [16, 4096, 1024], P(None, 'fs', 'tp'), may hold values from -0.09375 to 0.09375
- up_train: float32 [16, 4096, 1024], P(None, 'fs', 'tp'), may hold values from -0.09375 to 0.09375
- down_train: float32 [16, 1024, 4096], P(None, 'fs', 'tp'), may hold values from -0.1875 to 0.1875
Outputs:
- mixed: bfloat16 [4096, 4096], P('fs', 'tp')
- gate_new: bfloat16 [16, 4096, 1024], P('fs', None, 'tp')
- up_new: bfloat16 [16, 4096, 1024], P('fs', None, 'tp')
- down_new: bfloat16 [16, 1024, 4096], P('fs', 'tp')
The draws below stay inside these ranges and needn't reach their ends.
Inputs may be any that keep to these rules, and one draw needn't show every extreme that they name: `expert_ids`: each row names two different experts; within the rows of one index of fs no expert is named more than 96 times, a bound that some block reaches there.
All inputs are finite; a program needn't handle non-finite values.
Results may differ from the reference program's by a relative error of at most 0.0086.
Values may be sent and summed in bfloat16 or wider, within the bound.
A program may use at most 128 MiB of HBM per device.

```python
import math
import jax
import jax.numpy as jnp
import numpy as np
from jax import lax

D = 4096
FF = 1024
TOK_DEV = 512
EXPERTS = 16
TOKENS = 4096
CAP = 96
N_FS = 8


def levels(rng, extent, cuts, smallest, largest):
    gain = 1.0
    for position, shards_of in cuts:
        draws = jax.random.uniform(jax.random.fold_in(jax.random.fold_in(rng, 6), position), (shards_of,), jnp.float32, smallest / len(cuts), largest / len(cuts))
        gain = gain * jnp.repeat(jnp.exp(draws), extent[position] // shards_of).reshape((-1,) + (1,) * (len(extent) - 1 - position))
    return gain


def shared_out(rng, own, number, rows, count, top, most, skew):
    ranking = jax.random.permutation(rng, count)
    packed, ordinary = portions_of(count, rows * top, most, skew, True), portions_of(count, rows * top, most, skew, False)
    places = jnp.arange(count)

    def named(lengths, offset_by):
        used = int((lengths > 0).sum())
        fixed = max(1, used // 4)
        moved = fixed + (places - fixed + offset_by * (used - fixed)) % max(1, count - fixed)
        return jnp.zeros((count,), jnp.int32).at[ranking[jnp.where(places < fixed, places, moved)]].set(jnp.asarray(lengths, jnp.int32))

    lengths = jnp.where(number % 4 == 0, named(packed, number // 4), named(ordinary, number - number // 4 - 1))
    mixed = jax.random.permutation(jax.random.fold_in(own, 3), count)
    giver, sink = mixed[0:count // 2 * 2:2], mixed[1:count // 2 * 2:2]
    slack = jnp.minimum(lengths[giver] - 1, most - lengths[sink]) // 2
    slack = jnp.where((giver == ranking[0]) | (sink == ranking[0]) | (lengths[sink] == 0), 0, jnp.maximum(slack, 0))
    moved = jax.random.randint(jax.random.fold_in(own, 4), (count // 2,), 0, 1 << 20) % (slack + 1)
    lengths = lengths.at[giver].add(-moved).at[sink].add(moved)
    items = jnp.searchsorted(jnp.cumsum(lengths), jnp.arange(rows * top), side="right").astype(jnp.int32)
    grid = items.reshape(top, rows).T
    grid = grid[jax.random.permutation(jax.random.fold_in(own, 1), rows)]
    offset_by = jax.random.randint(jax.random.fold_in(own, 2), (rows, 1), 0, top)
    return jnp.take_along_axis(grid, (jnp.arange(top)[None, :] + offset_by) % top, axis=1)


def portions_of(count, total, reach, skew, full):
    portions = [(1 << 20) // math.isqrt(grade ** skew) + 1 for grade in range(1, count + 1)]
    largest = reach if full else min(reach, max(-(-total // count), total * portions[0] // sum(portions)))
    least = 1 if total - largest >= count - 1 else 0
    counts, spare = [largest] + [least] * (count - 1), total - largest - least * (count - 1)
    while spare > 0:
        candidates = [i for i in range(1, count) if counts[i] < largest] or [i for i in range(1, count) if counts[i] < reach]
        pool, remaining = sum([portions[i] for i in candidates]), spare
        for i in candidates:
            addition = min(reach - counts[i], max(1, remaining * portions[i] // pool), spare)
            counts[i] = counts[i] + addition
            spare = spare - addition
    return np.array(counts)


def bell_draw(rng, shape, spread, most, split=(), kind=jnp.bfloat16):
    array = spread * jax.random.normal(rng, shape, jnp.float32)
    if split:
        array = array * levels(rng, shape, split, -0.22, 0.18)
    return jnp.clip(array, -most, most).astype(kind)


def setup_inputs(seed: int = 0) -> dict:
    key_list = jax.random.split(jax.random.key(seed), 9)
    prompt = bell_draw(key_list[0], (TOKENS, D), 1.0, 6.0, ((0, 8),))
    expert_ids_keys = jax.random.split(jax.random.fold_in(key_list[1], 1), TOKENS // TOK_DEV)
    expert_ids_turns = jax.random.permutation(jax.random.fold_in(key_list[1], 3), TOKENS // TOK_DEV)
    expert_ids = jax.vmap(lambda own, number: shared_out(jax.random.fold_in(key_list[1], 2), own, number, TOK_DEV, EXPERTS, 2, CAP, 1))(expert_ids_keys, expert_ids_turns).reshape((TOKENS, 2))
    group_weight = jnp.clip(jnp.exp(math.log(1.0) - 1.3862944 * jax.random.uniform(key_list[2], (TOKENS,), jnp.float32) ** levels(key_list[2], (TOKENS,), ((0, 8),), -0.2, 0.2)), 0.25, 1.0)
    expert_share = jnp.clip(jnp.exp(math.log(1.0) - 2.3025851 * jax.random.uniform(key_list[3], (TOKENS, 2), jnp.float32) ** levels(key_list[3], (TOKENS, 2), ((0, 8),), -0.2, 0.2)), 0.1, 1.0)
    norm_gain = jnp.clip(1.0 + 0.18 * jax.random.normal(key_list[4], (D,), jnp.float32), 0.1, 1.9)
    gate_train = bell_draw(key_list[5], (EXPERTS, D, FF), D ** -0.5, 0.09375, ((1, 8), (2, 4)), jnp.float32)
    up_train = bell_draw(key_list[6], (EXPERTS, D, FF), D ** -0.5, 0.09375, ((1, 8), (2, 4)), jnp.float32)
    down_train = bell_draw(key_list[7], (EXPERTS, FF, D), FF ** -0.5, 0.1875, ((1, 8), (2, 4)), jnp.float32)
    return dict(prompt=prompt, expert_ids=expert_ids, group_weight=group_weight, expert_share=expert_share, norm_gain=norm_gain, gate_train=gate_train, up_train=up_train, down_train=down_train)


EPS = 1e-06

def reference(prompt, expert_ids, group_weight, expert_share, norm_gain, gate_train, up_train, down_train):
    gain_rows = norm_gain[None, :, None]
    gate_new = (gate_train * gain_rows).astype(jnp.bfloat16)
    up_new = (up_train * gain_rows).astype(jnp.bfloat16)
    down_new = down_train.astype(jnp.bfloat16)
    widened = prompt.astype(jnp.float32)
    normed = (widened * lax.rsqrt(lax.optimization_barrier(jnp.mean(widened * widened, axis=-1, keepdims=True)) + EPS)).astype(jnp.bfloat16)
    blocks = expert_ids.reshape(N_FS, TOK_DEV * 2)
    onehot = (blocks[:, :, None] == jnp.arange(EXPERTS, dtype=jnp.int32)[None, None, :]).astype(jnp.int32)
    slot_rank = lax.optimization_barrier(jnp.sum((jnp.cumsum(onehot, axis=1) - 1) * onehot, axis=2))
    slots = (jnp.arange(N_FS, dtype=jnp.int32)[:, None] * CAP + slot_rank).reshape(TOKENS, 2).astype(jnp.int32)
    token_rows = jnp.broadcast_to(normed[:, None, :], (TOKENS, 2, D))
    buffer = jnp.zeros((EXPERTS, N_FS * CAP, D), jnp.bfloat16).at[expert_ids, slots].set(token_rows)

    def expert(operands):
        expert_rows, w_gate, w_up, w_down = operands
        gate_val = jnp.dot(expert_rows, w_gate, preferred_element_type=jnp.float32)
        up_val = jnp.dot(expert_rows, w_up, preferred_element_type=jnp.float32)
        hidden = (jax.nn.silu(gate_val) * up_val).astype(jnp.bfloat16)
        return jnp.dot(hidden, w_down, preferred_element_type=jnp.float32).astype(jnp.bfloat16)
    outputs = lax.map(expert, (buffer, gate_new, up_new, down_new))
    picked = outputs[expert_ids, slots].astype(jnp.float32)
    weights = group_weight[:, None] * expert_share / lax.optimization_barrier(jnp.sum(expert_share, axis=1, keepdims=True))
    mixed = lax.optimization_barrier(jnp.sum(weights[:, :, None] * picked, axis=1)).astype(jnp.bfloat16)
    return (mixed, gate_new, up_new, down_new)
```

```python
import functools

import jax
import jax.numpy as jnp
from jax import lax
from jax.experimental import pallas as pl
from jax.experimental.pallas import tpu as pltpu
from jax.sharding import PartitionSpec as P

EPS = 1e-06
MESH = pl.DeviceIdType.MESH
BF16 = jnp.bfloat16
F32 = jnp.float32
PROMPT_STEPS = 4


def kernel(
    n,
    tp,
    prompt,
    ids,
    group,
    share,
    gain,
    gate_hbm,
    up_hbm,
    down_hbm,
    mixed_out,
    gate_out,
    up_out,
    down_out,
    wide,
    tall,
    gate_send,
    up_send,
    gate_land,
    up_land,
    down_land,
    rows_stage,
    piece,
    own_cols,
    far_cols,
    facts,
    far_facts,
    gain_cols,
    hid,
    gate_acc,
    spread,
    ret_stage,
    ret_land,
    far_stage,
    far_land,
    total,
    mixed_tile,
    load_sem,
    tall_sem,
    out_sem,
    send_sem,
    recv_sem,
    down_recv,
    chip_recv,
    mate_recv,
    hid_chip_recv,
    hid_mate_recv,
    ret_recv,
    far_recv,
):
    here = lax.axis_index("fs")
    me = lax.axis_index("tp")
    half = n // 2
    side = here // half
    seat = here % half
    partner = (here + half) % n
    mate = me + 1 - 2 * (me % 2)
    chips = tp // 2
    tokens, model_width = prompt.shape
    experts_all, depth, units = gate_hbm.shape
    local = experts_all // n
    capacity = ret_land.shape[4]
    own_width = own_cols.shape[1]
    down_depth = down_hbm.shape[1]
    chunks, width = down_land.shape[0], down_land.shape[3]
    seat_slots = local * capacity
    GATE, UP, DOWN, FACTS, COLS, ROWS, PIECE, HID, RET, FAR, TALL = range(11)

    def remote(src, dst, ssem, rsem, fs=None, tp_to=None):
        device = {"fs": here if fs is None else fs, "tp": me if tp_to is None else tp_to}
        return pltpu.make_async_remote_copy(
            src_ref=src,
            dst_ref=dst,
            send_sem=ssem,
            recv_sem=rsem,
            device_id=device,
            device_id_type=MESH,
        )

    def drain(ref, sem):
        pltpu.make_async_copy(ref, ref, sem).wait()

    def shift_of(k):
        return half + (k + 1) // 2 * (1 - 2 * (k % 2))

    def owner_of(k):
        return lax.rem(here + jnp.where(k == n - 1, 0, shift_of(k)), n)

    barrier = pltpu.get_barrier_semaphore()

    @pl.loop(1, n)
    def _(s):
        pl.semaphore_signal(
            barrier, inc=1, device_id={"fs": lax.rem(here + s, n), "tp": me}, device_id_type=MESH
        )

    @pl.loop(1, tp)
    def _(s):
        pl.semaphore_signal(
            barrier, inc=1, device_id={"fs": here, "tp": lax.rem(me + s, tp)}, device_id_type=MESH
        )

    def load(source, k):
        return pltpu.make_async_copy(
            source.at[pl.ds(owner_of(k) * local, local)], wide.at[k % 2], load_sem.at[k % 2]
        )

    def load_down(k, c):
        return pltpu.make_async_copy(
            down_hbm.at[pl.ds(owner_of(k) * local, local), :, pl.ds(c * width, width)],
            wide.at[k % 2, :, pl.ds(c * down_depth, down_depth), :],
            load_sem.at[k % 2],
        )

    block_rows = tokens // PROMPT_STEPS

    def load_prompt(i):
        return pltpu.make_async_copy(
            prompt.at[pl.ds(i * block_rows, block_rows)], tall.at[i % 2], tall_sem.at[i % 2]
        )

    load(gate_hbm, 0).start()
    load(gate_hbm, 1).start()
    load_prompt(0).start()
    load_prompt(1).start()

    lanes = min(128, depth)
    gain_cols[...] = jnp.transpose(jnp.broadcast_to(gain[...], (128, depth)))

    def cast(slot, out):
        for e in range(local):
            for j in range(units // 128):
                cols = pl.ds(j * 128, 128)
                out[e, :, cols] = (wide[slot, e, :, cols] * gain_cols[...]).astype(BF16)

    def send_weight(send, land, which, k):
        return remote(
            send.at[k],
            land.at[:, pl.ds(here * depth, depth), :],
            send_sem.at[which],
            recv_sem.at[which],
            fs=owner_of(k),
        )

    def weight_steps(source, send, land, which, first, last):
        @pl.loop(first, last)
        def _(k):
            load(source, k).wait()
            cast(k % 2, send.at[k])

            @pl.when(k + 2 < n)
            def _():
                load(source, k + 2).start()

            @pl.when(k > first)
            def _():
                send_weight(send, land, which, k - 1).start()

        send_weight(send, land, which, last - 1).start()

    def own_weight(source, land):
        load(source, n - 1).wait()
        cast((n - 1) % 2, land.at[:, pl.ds(here * depth, depth), :])

    for k in range(2):
        load(gate_hbm, k).wait()
        cast(k % 2, gate_send.at[k])
        load(gate_hbm, k + 2).start()
    pl.semaphore_wait(barrier, n - 1 + tp - 1)
    for k in range(2):
        send_weight(gate_send, gate_land, GATE, k).start()

    experts = lax.broadcasted_iota(jnp.int32, (experts_all, tokens), 0)
    named = [experts == ids[pl.ds(k, 1), :] for k in range(2)]
    count = sum(m.astype(F32) for m in named).astype(BF16)
    earlier = (
        lax.broadcasted_iota(jnp.int32, (tokens, tokens), 0)
        < lax.broadcasted_iota(jnp.int32, (tokens, tokens), 1)
    ).astype(F32).astype(BF16)
    ranks = jnp.dot(count, earlier, preferred_element_type=F32)
    shares = [share[pl.ds(k, 1), :] for k in range(2)]
    facts[...] = jnp.zeros_like(facts)
    for k in range(2):
        rank = jnp.sum(jnp.where(named[k], ranks, 0.0), axis=0, keepdims=True)
        facts[pl.ds(k, 1), :] = ids[pl.ds(k, 1), :].astype(F32) * capacity + rank
        facts[pl.ds(2 + k, 1), :] = group[...] * shares[k] / (shares[0] + shares[1])

    @pl.loop(0, PROMPT_STEPS)
    def _(i):
        load_prompt(i).wait()
        squares = jnp.zeros((block_rows, 128), F32)
        for j in range(model_width // 128):
            x = tall[i % 2, :, pl.ds(j * 128, 128)].astype(F32)
            squares += x * x
        mean = jnp.sum(squares, axis=1, keepdims=True) / model_width
        scale = lax.rsqrt(mean + EPS)
        cols = pl.ds(pl.multiple_of(me * own_width, 128), own_width)
        own_cols[pl.ds(pl.multiple_of(i * block_rows, block_rows), block_rows), :] = (
            tall[i % 2, :, cols].astype(F32) * scale
        ).astype(BF16)

        @pl.when(i + 2 < PROMPT_STEPS)
        def _():
            load_prompt(i + 2).start()

    send_facts = remote(
        facts, far_facts, send_sem.at[FACTS], recv_sem.at[FACTS], fs=partner
    )
    send_cols = remote(own_cols, far_cols, send_sem.at[COLS], recv_sem.at[COLS], fs=partner)
    send_facts.start()
    send_cols.start()

    weight_steps(gate_hbm, gate_send, gate_land, GATE, 2, n - 1)
    own_weight(gate_hbm, gate_land)
    load(up_hbm, 0).start()
    load(up_hbm, 1).start()

    def send_rows(q, j):
        to = lax.rem(seat + j, half)
        return remote(
            rows_stage.at[q, to],
            piece.at[me, :, pl.ds(pl.multiple_of((seat * 2 + q) * capacity, 16), capacity), :],
            send_sem.at[ROWS],
            recv_sem.at[ROWS],
            fs=side * half + to,
        )

    def place_rows(q, block_facts, columns):
        targets = [block_facts[pl.ds(k, 1), :].astype(jnp.int32) for k in range(2)]

        @pl.loop(0, half)
        def _(j):
            to = lax.rem(seat + j, half)
            slots = (side * half + to) * seat_slots + lax.broadcasted_iota(
                jnp.int32, (seat_slots, tokens), 0
            )
            picker = ((slots == targets[0]) | (slots == targets[1])).astype(F32).astype(BF16)
            rows = jnp.dot(picker, columns[...], preferred_element_type=F32)
            rows_stage[q, to] = rows.astype(BF16).reshape(local, capacity, own_width)

            @pl.when(j == 0)
            def _():
                piece[
                    me, :, pl.ds(pl.multiple_of((seat * 2 + q) * capacity, 16), capacity), :
                ] = rows_stage[q, seat]

            @pl.when(j > 1)
            def _():
                send_rows(q, j - 1).start()

        send_rows(q, half - 1).start()

    place_rows(0, facts, own_cols)
    send_facts.wait_recv()
    send_cols.wait_recv()
    place_rows(1, far_facts, far_cols)

    weight_steps(up_hbm, up_send, up_land, UP, 0, n - 1)
    own_weight(up_hbm, up_land)

    drain(gate_send, send_sem.at[GATE])

    @pl.loop(0, 2)
    def _(k):
        for c in range(chunks):
            load_down(k, c).start()

    def cast_down(k, out):
        for c in range(chunks):
            load_down(k, c).wait()
        for e in range(local):
            out[e] = wide[k % 2, e].astype(BF16)

        @pl.when(k + 2 < n)
        def _():
            for c in range(chunks):
                load_down(k + 2, c).start()

    @pl.loop(0, n - 1)
    def _(k):
        cast_down(k, gate_send.at[k])

    for c in range(chunks):
        load_down(n - 1, c).wait()
    for c in range(chunks):
        for e in range(local):
            down_land[c, e, pl.ds(pl.multiple_of(here * down_depth, 16), down_depth), :] = wide[
                (n - 1) % 2, e, pl.ds(c * down_depth, down_depth), :
            ].astype(BF16)

    @pl.loop(0, chunks)
    def _(c):
        @pl.loop(0, n - 1)
        def _(k):
            remote(
                gate_send.at[k, :, pl.ds(pl.multiple_of(c * down_depth, 16), down_depth), :],
                down_land.at[
                    c, :, pl.ds(pl.multiple_of(here * down_depth, 16), down_depth), :
                ],
                send_sem.at[DOWN],
                down_recv.at[c],
                fs=owner_of(k),
            ).start()

    def chip_peer(j):
        return lax.rem(me + 2 * j, tp)

    def chip_from(j):
        return lax.rem(me + tp - 2 * j, tp)

    def spread_tp(buffer, which, chip_sems, mate_sems):
        mine = buffer.at[me]

        @pl.loop(1, chips)
        def _(j):
            remote(mine, mine, send_sem.at[which], chip_sems.at[j - 1], tp_to=chip_peer(j)).start()

        remote(mine, mine, send_sem.at[which], mate_sems.at[0], tp_to=mate).start()

    def forward_tp(buffer, which, chip_sems, mate_sems):
        @pl.loop(1, chips)
        def _(j):
            theirs = buffer.at[chip_from(j)]
            pltpu.make_async_copy(theirs, theirs, chip_sems.at[j - 1]).wait()
            remote(theirs, theirs, send_sem.at[which], mate_sems.at[j], tp_to=mate).start()

    def collect_tp(buffer, mate_sems):
        @pl.loop(0, chips)
        def _(j):
            theirs = buffer.at[0]
            pltpu.make_async_copy(theirs, theirs, mate_sems.at[j]).wait()

    drain(
        piece.at[me, :, pl.ds(0, (half - 1) * 2 * capacity), :], recv_sem.at[ROWS]
    )
    spread_tp(piece, PIECE, chip_recv, mate_recv)

    @pl.loop(0, half)
    def _(j):
        for q in range(2):
            source = (facts, far_facts)[q]
            slots = (side * half + j) * seat_slots + lax.broadcasted_iota(
                jnp.int32, (seat_slots, tokens), 0
            )
            value = sum(
                jnp.where(
                    slots == source[pl.ds(k, 1), :].astype(jnp.int32),
                    source[pl.ds(2 + k, 1), :],
                    0.0,
                )
                for k in range(2)
            )
            high = value.astype(BF16)
            at = pl.ds(pl.multiple_of(j * seat_slots, 16), seat_slots)
            spread[q, 0, at, :] = high
            spread[q, 1, at, :] = (value - high.astype(F32)).astype(BF16)

    forward_tp(piece, PIECE, chip_recv, mate_recv)

    drain(gate_land.at[:, pl.ds(0, (n - 1) * depth), :], recv_sem.at[GATE])
    store_gate = pltpu.make_async_copy(gate_land, gate_out, out_sem.at[0])
    store_gate.start()
    collect_tp(piece, mate_recv)

    def contracted(land, e):
        acc = None
        for t in range(tp):
            part = jnp.dot(
                piece[t, e],
                land[e, pl.ds(t * own_width, own_width), :],
                preferred_element_type=F32,
            )
            acc = part if acc is None else acc + part
        return acc

    @pl.loop(0, local)
    def _(e):
        gate_acc[e] = contracted(gate_land, e)

    drain(up_land.at[:, pl.ds(0, (n - 1) * depth), :], recv_sem.at[UP])
    store_up = pltpu.make_async_copy(up_land, up_out, out_sem.at[1])
    store_up.start()

    @pl.loop(0, local)
    def _(e):
        g = gate_acc[e]
        hid[me, e] = (g / (1.0 + jnp.exp(-g)) * contracted(up_land, e)).astype(BF16)

    spread_tp(hid, HID, hid_chip_recv, hid_mate_recv)
    forward_tp(hid, HID, hid_chip_recv, hid_mate_recv)
    collect_tp(hid, hid_mate_recv)

    def down_cols(c, t):
        return down_out.at[
            :, :, pl.ds(pl.multiple_of(t * own_width + c * width, 128), width)
        ]

    def send_tall(c, j):
        to = lax.rem(me + j, tp)
        return remote(
            down_land.at[c, :, pl.ds(pl.multiple_of(to * units, 16), units), :],
            down_cols(c, me),
            send_sem.at[TALL],
            recv_sem.at[TALL],
            tp_to=to,
        )

    def own_tall(c):
        return pltpu.make_async_copy(
            down_land.at[c, :, pl.ds(pl.multiple_of(me * units, 16), units), :],
            down_cols(c, me),
            out_sem.at[2],
        )

    def send_back(c, q, j):
        to = lax.rem(seat + j, half)
        return remote(
            ret_stage.at[c, :, pl.ds(pl.multiple_of((to * 2 + q) * capacity, 16), capacity), :],
            ret_land.at[c, q, seat],
            send_sem.at[RET],
            ret_recv.at[c],
            fs=side * half + to,
        )

    def combine(c):
        drain(ret_land.at[c, :, pl.ds(0, half - 1)], ret_recv.at[c])
        for q in range(2):
            back = ret_land[c, q].reshape(half * seat_slots, width)
            value = sum(
                lax.dot_general(
                    spread[q, p], back, (((0,), (0,)), ((), ())), preferred_element_type=F32
                )
                for p in range(2)
            )
            if q:
                far_stage[c] = value.astype(BF16)
            else:
                total[c] = value

    def send_far(c):
        return remote(
            far_stage.at[c], far_land.at[c], send_sem.at[FAR], far_recv.at[c], fs=partner
        )

    @pl.loop(0, chunks)
    def _(c):
        drain(down_land.at[c, :, pl.ds(0, (n - 1) * down_depth), :], down_recv.at[c])

        @pl.loop(0, local)
        def _(e):
            acc = None
            for t in range(tp):
                part = jnp.dot(
                    hid[t, e],
                    down_land[c, e, pl.ds(t * units, units), :],
                    preferred_element_type=F32,
                )
                acc = part if acc is None else acc + part
            ret_stage[c, e] = acc.astype(BF16)

        own_tall(c).start()

        @pl.loop(1, tp)
        def _(j):
            send_tall(c, j).start()

        @pl.loop(1, half)
        def _(j):
            for q in range(2):
                send_back(c, q, j).start()

        for q in range(2):
            ret_land[c, q, seat] = ret_stage[
                c, :, pl.ds(pl.multiple_of((seat * 2 + q) * capacity, 16), capacity), :
            ]

        @pl.when(c > 0)
        def _():
            combine(c - 1)

        @pl.when(c > 0)
        def _():
            send_far(c - 1).start()

    combine(chunks - 1)

    def store_mixed(c):
        return pltpu.make_async_copy(
            mixed_tile.at[c],
            mixed_out.at[:, pl.ds(pl.multiple_of(c * width, 128), width)],
            out_sem.at[3],
        )

    @pl.loop(0, chunks)
    def _(c):
        @pl.when(c == 0)
        def _():
            send_far(chunks - 1).start()

        pltpu.make_async_copy(far_land.at[c], far_land.at[c], far_recv.at[c]).wait()
        mixed_tile[c] = (total[c] + far_land[c].astype(F32)).astype(BF16)
        store_mixed(c).start()

    drain(up_send, send_sem.at[UP])
    drain(gate_send, send_sem.at[DOWN])
    send_facts.wait_send()
    send_cols.wait_send()
    drain(piece.at[0, :, pl.ds(0, (half - 1) * 2 * capacity), :], send_sem.at[ROWS])
    drain(piece.at[pl.ds(0, 2 * chips - 1)], send_sem.at[PIECE])
    drain(hid.at[pl.ds(0, 2 * chips - 1)], send_sem.at[HID])
    drain(ret_land.at[:, :, pl.ds(0, half - 1)], send_sem.at[RET])
    drain(far_land, send_sem.at[FAR])
    others = down_out.at[:, :, pl.ds(0, (tp - 1) * own_width)]
    drain(others, send_sem.at[TALL])
    drain(others, recv_sem.at[TALL])
    drain(down_out.at[:, :, pl.ds(0, own_width)], out_sem.at[2])
    drain(mixed_tile, out_sem.at[3])
    store_gate.wait()
    store_up.wait()


def on_device(
    prompt, expert_ids, group_weight, expert_share, norm_gain, gate_train, up_train, down_train
):
    n = lax.axis_size("fs")
    tp = lax.axis_size("tp")
    half = n // 2
    tokens, model_width = prompt.shape
    experts_all, depth, units = gate_train.shape
    down_depth, own_width = down_train.shape[1:]
    local = experts_all // n
    hidden_width = n * down_depth
    capacity = max(2, 3 * tokens // experts_all)
    chunks = model_width // hidden_width
    width = own_width // chunks
    slots = half * 2 * capacity
    dma = pltpu.SemaphoreType.DMA
    scratch = [
        pltpu.VMEM((2, local, depth, units), F32),
        pltpu.VMEM((2, tokens // PROMPT_STEPS, model_width), BF16),
        pltpu.VMEM((n - 1, local, depth, units), BF16),
        pltpu.VMEM((n - 1, local, depth, units), BF16),
        pltpu.VMEM((local, n * depth, units), BF16),
        pltpu.VMEM((local, n * depth, units), BF16),
        pltpu.VMEM((chunks, local, hidden_width, width), BF16),
        pltpu.VMEM((2, half, local, capacity, own_width), BF16),
        pltpu.VMEM((tp, local, slots, own_width), BF16),
        pltpu.VMEM((tokens, own_width), BF16),
        pltpu.VMEM((tokens, own_width), BF16),
        pltpu.VMEM((8, tokens), F32),
        pltpu.VMEM((8, tokens), F32),
        pltpu.VMEM((depth, 128), F32),
        pltpu.VMEM((tp, local, slots, units), BF16),
        pltpu.VMEM((local, slots, units), F32),
        pltpu.VMEM((2, 2, half * local * capacity, tokens), BF16),
        pltpu.VMEM((chunks, local, slots, width), BF16),
        pltpu.VMEM((chunks, 2, half, local, capacity, width), BF16),
        pltpu.VMEM((chunks, tokens, width), BF16),
        pltpu.VMEM((chunks, tokens, width), BF16),
        pltpu.VMEM((chunks, tokens, width), F32),
        pltpu.VMEM((chunks, tokens, width), BF16),
        dma((2,)),
        dma((2,)),
        dma((4,)),
        dma((11,)),
        dma((11,)),
        dma((chunks,)),
        dma((max(1, tp // 2 - 1),)),
        dma((tp // 2,)),
        dma((max(1, tp // 2 - 1),)),
        dma((tp // 2,)),
        dma((chunks,)),
        dma((chunks,)),
    ]
    any_spec = pl.BlockSpec(memory_space=pl.ANY)
    vmem_spec = pl.BlockSpec(memory_space=pltpu.VMEM)
    return pl.pallas_call(
        functools.partial(kernel, n, tp),
        out_shape=(
            jax.ShapeDtypeStruct((tokens, own_width), BF16),
            jax.ShapeDtypeStruct((local, n * depth, units), BF16),
            jax.ShapeDtypeStruct((local, n * depth, units), BF16),
            jax.ShapeDtypeStruct((local, units, model_width), BF16),
        ),
        in_specs=[any_spec] + [vmem_spec] * 4 + [any_spec] * 3,
        out_specs=(any_spec,) * 4,
        scratch_shapes=scratch,
        compiler_params=pltpu.CompilerParams(
            collective_id=0, has_side_effects=True, vmem_limit_bytes=67043328
        ),
    )(
        prompt,
        expert_ids.T,
        group_weight[None, :],
        expert_share.T,
        norm_gain[None, :],
        gate_train,
        up_train,
        down_train,
    )


def solution(mesh):
    placed = (
        P("fs", None),
        P("fs", None),
        P("fs"),
        P("fs", None),
        P("fs"),
        P(None, "fs", "tp"),
        P(None, "fs", "tp"),
        P(None, "fs", "tp"),
    )
    return jax.shard_map(
        on_device,
        mesh=mesh,
        in_specs=placed,
        out_specs=(P("fs", "tp"), P("fs", None, "tp"), P("fs", None, "tp"), P("fs", "tp", None)),
        check_vma=False,
    )
```

```python
import functools

import jax
import jax.numpy as jnp
from jax import lax
from jax.experimental import pallas as pl
from jax.experimental.pallas import tpu as pltpu
from jax.sharding import PartitionSpec as P

EPS = 1e-06
MESH = pl.DeviceIdType.MESH
BF16 = jnp.bfloat16
F32 = jnp.float32
PROMPT_STEPS = 4
AHEAD = 2


def kernel(
    n,
    tp,
    prompt,
    ids,
    group,
    share,
    gain,
    gate_hbm,
    up_hbm,
    down_hbm,
    mixed_out,
    gate_land,
    up_land,
    down_out,
    wide,
    tall,
    sends,
    down_land,
    rows_stage,
    piece,
    own_cols,
    far_cols,
    facts,
    far_facts,
    gain_cols,
    hid,
    gate_acc,
    spread,
    ret_land,
    far_stage,
    far_land,
    total,
    load_sem,
    tall_sem,
    phase_send,
    phase_recv,
    down_recv,
    send_sem,
    recv_sem,
    rows_recv,
    chip_recv,
    mate_recv,
    hid_chip_recv,
    hid_mate_recv,
    ret_recv,
    last_ret_recv,
    far_recv,
):
    here = lax.axis_index("fs")
    me = lax.axis_index("tp")
    half = n // 2
    side = here // half
    seat = here % half
    partner = (here + half) % n
    mate = me + 1 - 2 * (me % 2)
    chips = tp // 2
    tokens, model_width = prompt.shape
    experts_all, depth, units = gate_hbm.shape
    local = experts_all // n
    last = local - 1
    capacity = ret_land.shape[3]
    own_width = own_cols.shape[1]
    down_depth = down_hbm.shape[1]
    chunks, width = down_land.shape[0], down_land.shape[3]
    seat_slots = local * capacity
    slots_of_seat = 2 * capacity
    buffers, slots_sent = wide.shape[0], sends.shape[0]
    FACTS, COLS, ROWS, PIECE, HID, RET, FAR, TALL = range(8)

    def remote(src, dst, ssem, rsem, fs=None, tp_to=None):
        device = {"fs": here if fs is None else fs, "tp": me if tp_to is None else tp_to}
        return pltpu.make_async_remote_copy(
            src_ref=src,
            dst_ref=dst,
            send_sem=ssem,
            recv_sem=rsem,
            device_id=device,
            device_id_type=MESH,
        )

    def drain(ref, sem):
        pltpu.make_async_copy(ref, ref, sem).wait()

    def at(start, size, step=16):
        return pl.ds(pl.multiple_of(start, step), size)

    def shift_of(k):
        return half + (k + 1) // 2 * (1 - 2 * (k % 2))

    def owner_of(k):
        return lax.rem(here + jnp.where(k == n - 1, 0, shift_of(k)), n)

    barrier = pltpu.get_barrier_semaphore()

    @pl.loop(1, n)
    def _(s):
        pl.semaphore_signal(
            barrier, inc=1, device_id={"fs": lax.rem(here + s, n), "tp": me}, device_id_type=MESH
        )

    @pl.loop(1, tp)
    def _(s):
        pl.semaphore_signal(
            barrier, inc=1, device_id={"fs": here, "tp": lax.rem(me + s, tp)}, device_id_type=MESH
        )

    def phase_of(e, kind):
        return 3 * e + kind

    def loads(e, kind, k):
        row = owner_of(k) * local + e
        slot = k % buffers
        if kind < 2:
            source = (gate_hbm, up_hbm)[kind]
            return [pltpu.make_async_copy(source.at[row], wide.at[slot], load_sem.at[slot])]
        return [
            pltpu.make_async_copy(
                down_hbm.at[row, :, pl.ds(c * width, width)],
                wide.at[slot, pl.ds(c * down_depth, down_depth), :],
                load_sem.at[slot],
            )
            for c in range(chunks)
        ]

    def start_loads(e, kind, k):
        for copy in loads(e, kind, k):
            copy.start()

    def wait_loads(k):
        drain(wide.at[k % buffers], load_sem.at[k % buffers])

    def cast(slot, kind):
        if kind == 2:
            return [(pl.ds(0, units), wide[slot].astype(BF16))]
        return [
            (
                pl.ds(j * 128, 128),
                (wide[slot, :, pl.ds(j * 128, 128)] * gain_cols[...]).astype(BF16),
            )
            for j in range(units // 128)
        ]

    def cast_step(e, kind, k):
        wait_loads(k)
        p = phase_of(e, kind) % slots_sent
        for cols, value in cast(k % buffers, kind):
            sends[p, k, :, cols] = value

        @pl.when(k + buffers < n)
        def _():
            start_loads(e, kind, k + buffers)

    def send_matrix(e, kind, k):
        p = phase_of(e, kind)
        land = (gate_land, up_land)[kind]
        remote(
            sends.at[p % slots_sent, k],
            land.at[e, at(here * depth, depth), :],
            phase_send.at[p],
            phase_recv.at[p],
            fs=owner_of(k),
        ).start()

    def send_down(e, c):
        p = phase_of(e, 2)

        @pl.loop(0, n - 1)
        def _(k):
            remote(
                sends.at[p % slots_sent, k, at(c * down_depth, down_depth), :],
                down_land.at[c, e, at(here * down_depth, down_depth), :],
                phase_send.at[p],
                down_recv.at[c] if e == last else phase_recv.at[p],
                fs=owner_of(k),
            ).start()

    def free_slot(p):
        if p >= slots_sent:
            drain(sends.at[p % slots_sent], phase_send.at[p - slots_sent])

    def own_block(e, kind):
        k = n - 1
        wait_loads(k)
        if kind < 2:
            land = (gate_land, up_land)[kind]
            for cols, value in cast(k % buffers, kind):
                land[e, at(here * depth, depth), cols] = value
            return
        for c in range(chunks):
            down_land[c, e, at(here * down_depth, down_depth), :] = wide[
                k % buffers, pl.ds(c * down_depth, down_depth), :
            ].astype(BF16)

    def begin(e, kind):
        for k in range(min(buffers, n)):
            start_loads(e, kind, k)

    def hand_over(e, kind, first=0):
        if not first:
            free_slot(phase_of(e, kind))
            begin(e, kind)

        @pl.loop(first, n - 1)
        def _(k):
            cast_step(e, kind, k)
            if kind < 2:

                @pl.when(k > first)
                def _():
                    send_matrix(e, kind, k - 1)

        if kind < 2:
            send_matrix(e, kind, n - 2)
        else:
            for c in range(min(AHEAD, chunks) if e == last else chunks):
                send_down(e, c)
        own_block(e, kind)

    block_rows = tokens // PROMPT_STEPS

    def load_prompt(i):
        return pltpu.make_async_copy(
            prompt.at[pl.ds(i * block_rows, block_rows)], tall.at[i % 2], tall_sem.at[i % 2]
        )

    begin(0, 0)
    load_prompt(0).start()
    load_prompt(1).start()
    gain_cols[...] = jnp.transpose(jnp.broadcast_to(gain[...], (128, depth)))

    for k in range(2):
        cast_step(0, 0, k)
    pl.semaphore_wait(barrier, n - 1 + tp - 1)
    for k in range(2):
        send_matrix(0, 0, k)

    experts = lax.broadcasted_iota(jnp.int32, (experts_all, tokens), 0)
    named = [experts == ids[pl.ds(k, 1), :] for k in range(2)]
    count = sum(m.astype(F32) for m in named).astype(BF16)
    earlier = (
        lax.broadcasted_iota(jnp.int32, (tokens, tokens), 0)
        < lax.broadcasted_iota(jnp.int32, (tokens, tokens), 1)
    ).astype(F32).astype(BF16)
    ranks = jnp.dot(count, earlier, preferred_element_type=F32)
    shares = [share[pl.ds(k, 1), :] for k in range(2)]
    facts[...] = jnp.zeros_like(facts)
    for k in range(2):
        rank = jnp.sum(jnp.where(named[k], ranks, 0.0), axis=0, keepdims=True)
        facts[pl.ds(k, 1), :] = ids[pl.ds(k, 1), :].astype(F32) * capacity + rank
        facts[pl.ds(2 + k, 1), :] = group[...] * shares[k] / (shares[0] + shares[1])

    @pl.loop(0, PROMPT_STEPS)
    def _(i):
        load_prompt(i).wait()
        squares = jnp.zeros((block_rows, 128), F32)
        for j in range(model_width // 128):
            x = tall[i % 2, :, pl.ds(j * 128, 128)].astype(F32)
            squares += x * x
        mean = jnp.sum(squares, axis=1, keepdims=True) / model_width
        scale = lax.rsqrt(mean + EPS)
        own_cols[at(i * block_rows, block_rows), :] = (
            tall[i % 2, :, at(me * own_width, own_width, 128)].astype(F32) * scale
        ).astype(BF16)

        @pl.when(i + 2 < PROMPT_STEPS)
        def _():
            load_prompt(i + 2).start()

    send_facts = remote(facts, far_facts, send_sem.at[FACTS], recv_sem.at[FACTS], fs=partner)
    send_cols = remote(own_cols, far_cols, send_sem.at[COLS], recv_sem.at[COLS], fs=partner)
    send_facts.start()
    send_cols.start()

    hand_over(0, 0, 2)

    def send_rows(q, j, e):
        to = lax.rem(seat + j, half)
        remote(
            rows_stage.at[q, to, e],
            piece.at[me, e, at((seat * 2 + q) * capacity, capacity), :],
            send_sem.at[ROWS],
            rows_recv.at[e],
            fs=side * half + to,
        ).start()

    def place_rows(q, block_facts, columns):
        targets = [block_facts[pl.ds(k, 1), :].astype(jnp.int32) for k in range(2)]

        @pl.loop(0, half)
        def _(j):
            to = lax.rem(seat + j, half)
            slots = (side * half + to) * seat_slots + lax.broadcasted_iota(
                jnp.int32, (seat_slots, tokens), 0
            )
            picker = ((slots == targets[0]) | (slots == targets[1])).astype(F32).astype(BF16)
            rows = jnp.dot(picker, columns[...], preferred_element_type=F32)
            rows_stage[q, to] = rows.astype(BF16).reshape(local, capacity, own_width)

            @pl.when(j == 0)
            def _():
                piece[me, :, at((seat * 2 + q) * capacity, capacity), :] = rows_stage[q, seat]

        for e in range(local):

            @pl.loop(1, half)
            def _(j):
                send_rows(q, j, e)

    place_rows(0, facts, own_cols)
    send_facts.wait_recv()
    send_cols.wait_recv()
    place_rows(1, far_facts, far_cols)

    hand_over(0, 1)
    hand_over(0, 2)

    def spread_tp(buffer, e, which, chip_sems, mate_sems):
        mine = buffer.at[me, e]

        @pl.loop(1, chips)
        def _(j):
            remote(
                mine,
                mine,
                send_sem.at[which],
                chip_sems.at[e, j - 1],
                tp_to=lax.rem(me + 2 * j, tp),
            ).start()

        remote(mine, mine, send_sem.at[which], mate_sems.at[e, 0], tp_to=mate).start()

    def forward_tp(buffer, e, which, chip_sems, mate_sems):
        @pl.loop(1, chips)
        def _(j):
            theirs = buffer.at[lax.rem(me + tp - 2 * j, tp), e]
            drain(theirs, chip_sems.at[e, j - 1])
            remote(theirs, theirs, send_sem.at[which], mate_sems.at[e, j], tp_to=mate).start()

    def collect_tp(buffer, e, mate_sems):
        @pl.loop(0, chips)
        def _(j):
            drain(buffer.at[0, e], mate_sems.at[e, j])

    for e in range(local):
        drain(piece.at[me, e, pl.ds(0, (half - 1) * slots_of_seat), :], rows_recv.at[e])
        spread_tp(piece, e, PIECE, chip_recv, mate_recv)

    if local > 1:
        hand_over(1, 0)
        hand_over(1, 1)

    @pl.loop(0, half)
    def _(j):
        for q in range(2):
            source = (facts, far_facts)[q]
            slots = (side * half + j) * seat_slots + lax.broadcasted_iota(
                jnp.int32, (seat_slots, tokens), 0
            )
            value = sum(
                jnp.where(
                    slots == source[pl.ds(k, 1), :].astype(jnp.int32),
                    source[pl.ds(2 + k, 1), :],
                    0.0,
                )
                for k in range(2)
            )
            high = value.astype(BF16)
            spread[q, 0, at(j * seat_slots, seat_slots), :] = high
            spread[q, 1, at(j * seat_slots, seat_slots), :] = (value - high.astype(F32)).astype(
                BF16
            )

    drain(rows_stage.at[:, pl.ds(0, half - 1)], send_sem.at[ROWS])

    def contracted(land, e):
        acc = None
        for t in range(tp):
            part = jnp.dot(
                piece[t, e],
                land[e, pl.ds(t * own_width, own_width), :],
                preferred_element_type=F32,
            )
            acc = part if acc is None else acc + part
        return acc

    def hidden(e):
        forward_tp(piece, e, PIECE, chip_recv, mate_recv)
        drain(gate_land.at[e, pl.ds(0, (n - 1) * depth), :], phase_recv.at[phase_of(e, 0)])
        collect_tp(piece, e, mate_recv)
        gate_acc[...] = contracted(gate_land, e)
        drain(up_land.at[e, pl.ds(0, (n - 1) * depth), :], phase_recv.at[phase_of(e, 1)])
        up_val = contracted(up_land, e)
        g = gate_acc[...]
        hid[me, e] = (g / (1.0 + jnp.exp(-g)) * up_val).astype(BF16)
        spread_tp(hid, e, HID, hid_chip_recv, hid_mate_recv)
        forward_tp(hid, e, HID, hid_chip_recv, hid_mate_recv)
        collect_tp(hid, e, hid_mate_recv)

    def down_cols(c, e, t):
        return down_out.at[e, :, at(t * own_width + c * width, width, 128)]

    def expert_out(c, e):
        acc = None
        for t in range(tp):
            part = jnp.dot(
                hid[t, e],
                down_land[c, e, pl.ds(t * units, units), :],
                preferred_element_type=F32,
            )
            acc = part if acc is None else acc + part
        out = acc.astype(BF16).reshape(half, 2, capacity, width)
        for m in range(half):
            for q in range(2):
                rows_stage[q, m, e, :, at(c * width, width, 128)] = out[m, q]

    def turn_down(c, e):
        down_out[e, :, at(me * own_width + c * width, width, 128)] = down_land[
            c, e, at(me * units, units), :
        ]

        @pl.loop(1, tp)
        def _(j):
            to = lax.rem(me + j, tp)
            remote(
                down_land.at[c, e, at(to * units, units), :],
                down_cols(c, e, me),
                send_sem.at[TALL],
                recv_sem.at[TALL],
                tp_to=to,
            ).start()

    def send_back(e, cols, rsem):
        for q in range(2):

            @pl.loop(1, half)
            def _(j):
                to = lax.rem(seat + j, half)
                remote(
                    rows_stage.at[q, to, e, :, cols],
                    ret_land.at[q, seat, e, :, cols],
                    send_sem.at[RET],
                    rsem,
                    fs=side * half + to,
                ).start()

        for q in range(2):
            ret_land[q, seat, e, :, cols] = rows_stage[q, seat, e, :, cols]

    for e in range(last):
        hidden(e)
        p = phase_of(e, 2)
        drain(down_land.at[:, e, pl.ds(0, (n - 1) * down_depth), :], phase_recv.at[p])

        @pl.loop(0, chunks)
        def _(c):
            expert_out(c, e)

        send_back(e, pl.ds(0, own_width), ret_recv.at[e])
        hand_over(e + 1, 2)

        @pl.loop(0, chunks)
        def _(c):
            turn_down(c, e)

        if e + 2 < local:
            hand_over(e + 2, 0)
            hand_over(e + 2, 1)

    hidden(last)
    for e in range(last):
        drain(ret_land.at[:, pl.ds(0, half - 1), e], ret_recv.at[e])

    def combine(c):
        cols = at(c * width, width, 128)
        drain(ret_land.at[:, pl.ds(0, half - 1), last, :, cols], last_ret_recv.at[c])
        for q in range(2):
            back = ret_land[q, :, :, :, cols].reshape(half * seat_slots, width)
            value = sum(
                lax.dot_general(
                    spread[q, p], back, (((0,), (0,)), ((), ())), preferred_element_type=F32
                )
                for p in range(2)
            )
            if q:
                far_stage[c] = value.astype(BF16)
            else:
                total[c] = value

    def send_far(c):
        remote(
            far_stage.at[c], far_land.at[c], send_sem.at[FAR], far_recv.at[c], fs=partner
        ).start()

    @pl.loop(0, chunks)
    def _(c):
        drain(down_land.at[c, last, pl.ds(0, (n - 1) * down_depth), :], down_recv.at[c])
        expert_out(c, last)
        send_back(last, at(c * width, width, 128), last_ret_recv.at[c])

        @pl.when(c + AHEAD < chunks)
        def _():
            send_down(last, c + AHEAD)

        turn_down(c, last)

        @pl.when(c > 0)
        def _():
            combine(c - 1)
            send_far(c - 1)

    combine(chunks - 1)
    send_far(chunks - 1)

    @pl.loop(0, chunks)
    def _(c):
        drain(far_land.at[c], far_recv.at[c])
        mixed_out[:, at(c * width, width, 128)] = (
            total[c] + far_land[c].astype(F32)
        ).astype(BF16)

    for p in range(max(0, 3 * local - slots_sent), 3 * local):
        drain(sends.at[p % slots_sent], phase_send.at[p])
    send_facts.wait_send()
    send_cols.wait_send()
    drain(piece.at[pl.ds(0, 2 * chips - 1)], send_sem.at[PIECE])
    drain(hid.at[pl.ds(0, 2 * chips - 1)], send_sem.at[HID])
    drain(ret_land.at[:, pl.ds(0, half - 1)], send_sem.at[RET])
    drain(far_land, send_sem.at[FAR])
    others = down_out.at[:, :, pl.ds(0, (tp - 1) * own_width)]
    drain(others, send_sem.at[TALL])
    drain(others, recv_sem.at[TALL])


def on_device(
    prompt, expert_ids, group_weight, expert_share, norm_gain, gate_train, up_train, down_train
):
    n = lax.axis_size("fs")
    tp = lax.axis_size("tp")
    half = n // 2
    tokens, model_width = prompt.shape
    experts_all, depth, units = gate_train.shape
    down_depth, own_width = down_train.shape[1:]
    local = experts_all // n
    hidden_width = n * down_depth
    capacity = max(2, 3 * tokens // experts_all)
    chunks = model_width // hidden_width
    width = own_width // chunks
    slots = half * 2 * capacity
    dma = pltpu.SemaphoreType.DMA
    scratch = [
        pltpu.VMEM((4, depth, units), F32),
        pltpu.VMEM((2, tokens // PROMPT_STEPS, model_width), BF16),
        pltpu.VMEM((4, n - 1, depth, units), BF16),
        pltpu.VMEM((chunks, local, hidden_width, width), BF16),
        pltpu.VMEM((2, half, local, capacity, own_width), BF16),
        pltpu.VMEM((tp, local, slots, own_width), BF16),
        pltpu.VMEM((tokens, own_width), BF16),
        pltpu.VMEM((tokens, own_width), BF16),
        pltpu.VMEM((8, tokens), F32),
        pltpu.VMEM((8, tokens), F32),
        pltpu.VMEM((depth, 128), F32),
        pltpu.VMEM((tp, local, slots, units), BF16),
        pltpu.VMEM((slots, units), F32),
        pltpu.VMEM((2, 2, half * local * capacity, tokens), BF16),
        pltpu.VMEM((2, half, local, capacity, own_width), BF16),
        pltpu.VMEM((chunks, tokens, width), BF16),
        pltpu.VMEM((chunks, tokens, width), BF16),
        pltpu.VMEM((chunks, tokens, width), F32),
        dma((4,)),
        dma((2,)),
        dma((3 * local,)),
        dma((3 * local,)),
        dma((chunks,)),
        dma((8,)),
        dma((8,)),
        dma((local,)),
        dma((local, max(1, tp // 2 - 1))),
        dma((local, tp // 2)),
        dma((local, max(1, tp // 2 - 1))),
        dma((local, tp // 2)),
        dma((max(1, local - 1),)),
        dma((chunks,)),
        dma((chunks,)),
    ]
    any_spec = pl.BlockSpec(memory_space=pl.ANY)
    vmem_spec = pl.BlockSpec(memory_space=pltpu.VMEM)
    return pl.pallas_call(
        functools.partial(kernel, n, tp),
        out_shape=(
            pltpu.VMEM((tokens, own_width), BF16),
            pltpu.VMEM((local, n * depth, units), BF16),
            pltpu.VMEM((local, n * depth, units), BF16),
            pltpu.VMEM((local, units, model_width), BF16),
        ),
        in_specs=[any_spec] + [vmem_spec] * 4 + [any_spec] * 3,
        out_specs=(vmem_spec,) * 4,
        scratch_shapes=scratch,
        compiler_params=pltpu.CompilerParams(
            collective_id=0, has_side_effects=True, vmem_limit_bytes=49 << 20
        ),
    )(
        prompt,
        expert_ids.T,
        group_weight[None, :],
        expert_share.T,
        norm_gain[None, :],
        gate_train,
        up_train,
        down_train,
    )


def solution(mesh):
    placed = (
        P("fs", None),
        P("fs", None),
        P("fs"),
        P("fs", None),
        P("fs"),
        P(None, "fs", "tp"),
        P(None, "fs", "tp"),
        P(None, "fs", "tp"),
    )
    return jax.shard_map(
        on_device,
        mesh=mesh,
        in_specs=placed,
        out_specs=(P("fs", "tp"), P("fs", None, "tp"), P("fs", None, "tp"), P("fs", "tp", None)),
        check_vma=False,
    )
```

```python
import functools

import jax
import jax.numpy as jnp
from jax import lax
from jax.experimental import pallas as pl
from jax.experimental.pallas import tpu as pltpu
from jax.sharding import PartitionSpec as P

EPS = 1e-06
MESH = pl.DeviceIdType.MESH
BF16 = jnp.bfloat16
F32 = jnp.float32
PROMPT_STEPS = 4
AHEAD = 2


def kernel(
    n,
    tp,
    prompt,
    ids,
    group,
    share,
    gain,
    gate_hbm,
    up_hbm,
    down_hbm,
    mixed_out,
    gate_land,
    up_land,
    down_out,
    wide,
    tall,
    sends,
    down_land,
    rows_stage,
    piece,
    own_cols,
    far_cols,
    facts,
    far_facts,
    gain_cols,
    hid,
    gate_acc,
    spread,
    ret_land,
    far_stage,
    far_land,
    total,
    load_sem,
    tall_sem,
    phase_send,
    phase_recv,
    down_recv,
    send_sem,
    recv_sem,
    rows_recv,
    chip_recv,
    mate_recv,
    hid_chip_recv,
    hid_mate_recv,
    ret_recv,
    last_ret_recv,
    far_recv,
):
    here = lax.axis_index("fs")
    me = lax.axis_index("tp")
    half = n // 2
    side = here // half
    seat = here % half
    partner = (here + half) % n
    mate = me + 1 - 2 * (me % 2)
    chips = tp // 2
    tokens, model_width = prompt.shape
    experts_all, depth, units = gate_hbm.shape
    local = experts_all // n
    last = local - 1
    capacity = ret_land.shape[3]
    own_width = own_cols.shape[1]
    down_depth = down_hbm.shape[1]
    chunks, width = down_land.shape[0], down_land.shape[3]
    seat_slots = local * capacity
    slots_of_seat = 2 * capacity
    buffers, slots_sent = wide.shape[0], sends.shape[0]
    FACTS, COLS, ROWS, PIECE, HID, RET, FAR, TALL = range(8)

    def remote(src, dst, ssem, rsem, fs=None, tp_to=None):
        device = {"fs": here if fs is None else fs, "tp": me if tp_to is None else tp_to}
        return pltpu.make_async_remote_copy(
            src_ref=src,
            dst_ref=dst,
            send_sem=ssem,
            recv_sem=rsem,
            device_id=device,
            device_id_type=MESH,
        )

    def drain(ref, sem):
        pltpu.make_async_copy(ref, ref, sem).wait()

    def at(start, size, step=16):
        return pl.ds(pl.multiple_of(start, step), size)

    def shift_of(k):
        return half + (k + 1) // 2 * (1 - 2 * (k % 2))

    def owner_of(k):
        return lax.rem(here + jnp.where(k == n - 1, 0, shift_of(k)), n)

    barrier = pltpu.get_barrier_semaphore()

    @pl.loop(1, n)
    def _(s):
        pl.semaphore_signal(
            barrier, inc=1, device_id={"fs": lax.rem(here + s, n), "tp": me}, device_id_type=MESH
        )

    @pl.loop(1, tp)
    def _(s):
        pl.semaphore_signal(
            barrier, inc=1, device_id={"fs": here, "tp": lax.rem(me + s, tp)}, device_id_type=MESH
        )

    def phase_of(e, kind):
        return 3 * e + kind

    def loads(e, kind, k):
        row = owner_of(k) * local + e
        slot = k % buffers
        if kind < 2:
            source = (gate_hbm, up_hbm)[kind]
            return [pltpu.make_async_copy(source.at[row], wide.at[slot], load_sem.at[slot])]
        return [
            pltpu.make_async_copy(
                down_hbm.at[row, :, pl.ds(c * width, width)],
                wide.at[slot, pl.ds(c * down_depth, down_depth), :],
                load_sem.at[slot],
            )
            for c in range(chunks)
        ]

    def start_loads(e, kind, k):
        for copy in loads(e, kind, k):
            copy.start()

    def wait_loads(k):
        drain(wide.at[k % buffers], load_sem.at[k % buffers])

    def cast(slot, kind):
        if kind == 2:
            return [(pl.ds(0, units), wide[slot].astype(BF16))]
        return [
            (
                pl.ds(j * 128, 128),
                (wide[slot, :, pl.ds(j * 128, 128)] * gain_cols[...]).astype(BF16),
            )
            for j in range(units // 128)
        ]

    def cast_step(e, kind, k):
        wait_loads(k)
        p = phase_of(e, kind) % slots_sent
        for cols, value in cast(k % buffers, kind):
            sends[p, k, :, cols] = value

        @pl.when(k + buffers < n)
        def _():
            start_loads(e, kind, k + buffers)

    def send_matrix(e, kind, k):
        p = phase_of(e, kind)
        land = (gate_land, up_land)[kind]
        remote(
            sends.at[p % slots_sent, k],
            land.at[e, at(here * depth, depth), :],
            phase_send.at[p],
            phase_recv.at[p],
            fs=owner_of(k),
        ).start()

    def send_down(e, c):
        p = phase_of(e, 2)

        @pl.loop(0, n - 1)
        def _(k):
            remote(
                sends.at[p % slots_sent, k, at(c * down_depth, down_depth), :],
                down_land.at[c, e, at(here * down_depth, down_depth), :],
                phase_send.at[p],
                down_recv.at[c] if e == last else phase_recv.at[p],
                fs=owner_of(k),
            ).start()

    def free_slot(p):
        if p >= slots_sent:
            drain(sends.at[p % slots_sent], phase_send.at[p - slots_sent])

    def own_block(e, kind):
        k = n - 1
        wait_loads(k)
        if kind < 2:
            land = (gate_land, up_land)[kind]
            for cols, value in cast(k % buffers, kind):
                land[e, at(here * depth, depth), cols] = value
            return
        for c in range(chunks):
            down_land[c, e, at(here * down_depth, down_depth), :] = wide[
                k % buffers, pl.ds(c * down_depth, down_depth), :
            ].astype(BF16)

    def begin(e, kind):
        for k in range(min(buffers, n)):
            start_loads(e, kind, k)

    def hand_over(e, kind, first=0):
        if not first:
            free_slot(phase_of(e, kind))
            begin(e, kind)

        @pl.loop(first, n - 1)
        def _(k):
            cast_step(e, kind, k)
            if kind < 2:

                @pl.when(k > first)
                def _():
                    send_matrix(e, kind, k - 1)

        if kind < 2:
            send_matrix(e, kind, n - 2)
        else:
            for c in range(min(AHEAD, chunks) if e == last else chunks):
                send_down(e, c)
        own_block(e, kind)

    block_rows = tokens // PROMPT_STEPS

    def load_prompt(i):
        return pltpu.make_async_copy(
            prompt.at[pl.ds(i * block_rows, block_rows)], tall.at[i % 2], tall_sem.at[i % 2]
        )

    begin(0, 0)
    load_prompt(0).start()
    load_prompt(1).start()
    gain_cols[...] = jnp.transpose(jnp.broadcast_to(gain[...], (128, depth)))

    for k in range(2):
        cast_step(0, 0, k)
    pl.semaphore_wait(barrier, n - 1 + tp - 1)
    for k in range(2):
        send_matrix(0, 0, k)

    experts = lax.broadcasted_iota(jnp.int32, (experts_all, tokens), 0)
    named = [experts == ids[pl.ds(k, 1), :] for k in range(2)]
    count = sum(m.astype(F32) for m in named).astype(BF16)
    earlier = (
        lax.broadcasted_iota(jnp.int32, (tokens, tokens), 0)
        < lax.broadcasted_iota(jnp.int32, (tokens, tokens), 1)
    ).astype(F32).astype(BF16)
    ranks = jnp.dot(count, earlier, preferred_element_type=F32)
    shares = [share[pl.ds(k, 1), :] for k in range(2)]
    facts[...] = jnp.zeros_like(facts)
    for k in range(2):
        rank = jnp.sum(jnp.where(named[k], ranks, 0.0), axis=0, keepdims=True)
        facts[pl.ds(k, 1), :] = ids[pl.ds(k, 1), :].astype(F32) * capacity + rank
        facts[pl.ds(2 + k, 1), :] = group[...] * shares[k] / (shares[0] + shares[1])

    @pl.loop(0, PROMPT_STEPS)
    def _(i):
        load_prompt(i).wait()
        squares = jnp.zeros((block_rows, 128), F32)
        for j in range(model_width // 128):
            x = tall[i % 2, :, pl.ds(j * 128, 128)].astype(F32)
            squares += x * x
        mean = jnp.sum(squares, axis=1, keepdims=True) / model_width
        scale = lax.rsqrt(mean + EPS)
        own_cols[at(i * block_rows, block_rows), :] = (
            tall[i % 2, :, at(me * own_width, own_width, 128)].astype(F32) * scale
        ).astype(BF16)

        @pl.when(i + 2 < PROMPT_STEPS)
        def _():
            load_prompt(i + 2).start()

    send_facts = remote(facts, far_facts, send_sem.at[FACTS], recv_sem.at[FACTS], fs=partner)
    send_cols = remote(own_cols, far_cols, send_sem.at[COLS], recv_sem.at[COLS], fs=partner)
    send_facts.start()
    send_cols.start()

    hand_over(0, 0, 2)

    def send_rows(q, j, e):
        to = lax.rem(seat + j, half)
        remote(
            rows_stage.at[q, to, e],
            piece.at[me, e, at((seat * 2 + q) * capacity, capacity), :],
            send_sem.at[ROWS],
            rows_recv.at[e],
            fs=side * half + to,
        ).start()

    def place_rows(q, block_facts, columns):
        targets = [block_facts[pl.ds(k, 1), :].astype(jnp.int32) for k in range(2)]

        @pl.loop(0, half)
        def _(j):
            to = lax.rem(seat + j, half)
            slots = (side * half + to) * seat_slots + lax.broadcasted_iota(
                jnp.int32, (seat_slots, tokens), 0
            )
            picker = ((slots == targets[0]) | (slots == targets[1])).astype(F32).astype(BF16)
            rows = jnp.dot(picker, columns[...], preferred_element_type=F32)
            rows_stage[q, to] = rows.astype(BF16).reshape(local, capacity, own_width)

            @pl.when(j == 0)
            def _():
                piece[me, :, at((seat * 2 + q) * capacity, capacity), :] = rows_stage[q, seat]

        for e in range(local):

            @pl.loop(1, half)
            def _(j):
                send_rows(q, j, e)

    place_rows(0, facts, own_cols)
    send_facts.wait_recv()
    send_cols.wait_recv()
    place_rows(1, far_facts, far_cols)

    hand_over(0, 1)
    hand_over(0, 2)

    def spread_tp(buffer, e, which, chip_sems, mate_sems):
        mine = buffer.at[me, e]

        @pl.loop(1, chips)
        def _(j):
            remote(
                mine,
                mine,
                send_sem.at[which],
                chip_sems.at[e, j - 1],
                tp_to=lax.rem(me + 2 * j, tp),
            ).start()

        remote(mine, mine, send_sem.at[which], mate_sems.at[e, 0], tp_to=mate).start()

    def forward_tp(buffer, e, which, chip_sems, mate_sems):
        @pl.loop(1, chips)
        def _(j):
            theirs = buffer.at[lax.rem(me + tp - 2 * j, tp), e]
            drain(theirs, chip_sems.at[e, j - 1])
            remote(theirs, theirs, send_sem.at[which], mate_sems.at[e, j], tp_to=mate).start()

    def collect_tp(buffer, e, mate_sems):
        @pl.loop(0, chips)
        def _(j):
            drain(buffer.at[0, e], mate_sems.at[e, j])

    for e in range(local):
        drain(piece.at[me, e, pl.ds(0, (half - 1) * slots_of_seat), :], rows_recv.at[e])
        spread_tp(piece, e, PIECE, chip_recv, mate_recv)

    if local > 1:
        hand_over(1, 0)
        hand_over(1, 1)

    @pl.loop(0, half)
    def _(j):
        for q in range(2):
            source = (facts, far_facts)[q]
            slots = (side * half + j) * seat_slots + lax.broadcasted_iota(
                jnp.int32, (seat_slots, tokens), 0
            )
            value = sum(
                jnp.where(
                    slots == source[pl.ds(k, 1), :].astype(jnp.int32),
                    source[pl.ds(2 + k, 1), :],
                    0.0,
                )
                for k in range(2)
            )
            high = value.astype(BF16)
            spread[q, 0, at(j * seat_slots, seat_slots), :] = high
            spread[q, 1, at(j * seat_slots, seat_slots), :] = (value - high.astype(F32)).astype(
                BF16
            )

    drain(rows_stage.at[:, pl.ds(0, half - 1)], send_sem.at[ROWS])

    def contracted(land, e):
        acc = None
        for t in range(tp):
            part = jnp.dot(
                piece[t, e],
                land[e, pl.ds(t * own_width, own_width), :],
                preferred_element_type=F32,
            )
            acc = part if acc is None else acc + part
        return acc

    def hidden(e):
        forward_tp(piece, e, PIECE, chip_recv, mate_recv)
        drain(gate_land.at[e, pl.ds(0, (n - 1) * depth), :], phase_recv.at[phase_of(e, 0)])
        collect_tp(piece, e, mate_recv)
        gate_acc[...] = contracted(gate_land, e)
        drain(up_land.at[e, pl.ds(0, (n - 1) * depth), :], phase_recv.at[phase_of(e, 1)])
        up_val = contracted(up_land, e)
        g = gate_acc[...]
        hid[me, e] = (g / (1.0 + jnp.exp(-g)) * up_val).astype(BF16)
        spread_tp(hid, e, HID, hid_chip_recv, hid_mate_recv)
        forward_tp(hid, e, HID, hid_chip_recv, hid_mate_recv)
        collect_tp(hid, e, hid_mate_recv)

    def down_cols(c, e, t):
        return down_out.at[e, :, at(t * own_width + c * width, width, 128)]

    def expert_out(c, e):
        acc = None
        for t in range(tp):
            part = jnp.dot(
                hid[t, e],
                down_land[c, e, pl.ds(t * units, units), :],
                preferred_element_type=F32,
            )
            acc = part if acc is None else acc + part
        out = acc.astype(BF16).reshape(half, 2, capacity, width)
        for m in range(half):
            for q in range(2):
                rows_stage[q, m, e, :, at(c * width, width, 128)] = out[m, q]

    def turn_down(c, e):
        down_out[e, :, at(me * own_width + c * width, width, 128)] = down_land[
            c, e, at(me * units, units), :
        ]

        @pl.loop(1, tp)
        def _(j):
            to = lax.rem(me + j, tp)
            remote(
                down_land.at[c, e, at(to * units, units), :],
                down_cols(c, e, me),
                send_sem.at[TALL],
                recv_sem.at[TALL],
                tp_to=to,
            ).start()

    def send_back(e, cols, rsem):
        for q in range(2):

            @pl.loop(1, half)
            def _(j):
                to = lax.rem(seat + j, half)
                remote(
                    rows_stage.at[q, to, e, :, cols],
                    ret_land.at[q, seat, e, :, cols],
                    send_sem.at[RET],
                    rsem,
                    fs=side * half + to,
                ).start()

        for q in range(2):
            ret_land[q, seat, e, :, cols] = rows_stage[q, seat, e, :, cols]

    for e in range(last):
        hidden(e)
        p = phase_of(e, 2)
        drain(down_land.at[:, e, pl.ds(0, (n - 1) * down_depth), :], phase_recv.at[p])

        @pl.loop(0, chunks)
        def _(c):
            expert_out(c, e)

        send_back(e, pl.ds(0, own_width), ret_recv.at[e])
        hand_over(e + 1, 2)

        @pl.loop(0, chunks)
        def _(c):
            turn_down(c, e)

        if e + 2 < local:
            hand_over(e + 2, 0)
            hand_over(e + 2, 1)

    hidden(last)
    for e in range(last):
        drain(ret_land.at[:, pl.ds(0, half - 1), e], ret_recv.at[e])

    def combine(c):
        cols = at(c * width, width, 128)
        drain(ret_land.at[:, pl.ds(0, half - 1), last, :, cols], last_ret_recv.at[c])
        for q in range(2):
            back = ret_land[q, :, :, :, cols].reshape(half * seat_slots, width)
            value = sum(
                lax.dot_general(
                    spread[q, p], back, (((0,), (0,)), ((), ())), preferred_element_type=F32
                )
                for p in range(2)
            )
            if q:
                far_stage[c] = value.astype(BF16)
            else:
                total[c] = value

    def send_far(c):
        remote(
            far_stage.at[c], far_land.at[c], send_sem.at[FAR], far_recv.at[c], fs=partner
        ).start()

    @pl.loop(0, chunks)
    def _(c):
        drain(down_land.at[c, last, pl.ds(0, (n - 1) * down_depth), :], down_recv.at[c])
        expert_out(c, last)
        send_back(last, at(c * width, width, 128), last_ret_recv.at[c])

        @pl.when(c + AHEAD < chunks)
        def _():
            send_down(last, c + AHEAD)

        turn_down(c, last)

        @pl.when(c > 0)
        def _():
            combine(c - 1)
            send_far(c - 1)

    combine(chunks - 1)
    send_far(chunks - 1)

    @pl.loop(0, chunks)
    def _(c):
        drain(far_land.at[c], far_recv.at[c])
        mixed_out[:, at(c * width, width, 128)] = (
            total[c] + far_land[c].astype(F32)
        ).astype(BF16)

    for p in range(max(0, 3 * local - slots_sent), 3 * local):
        drain(sends.at[p % slots_sent], phase_send.at[p])
    send_facts.wait_send()
    send_cols.wait_send()
    drain(piece.at[pl.ds(0, 2 * chips - 1)], send_sem.at[PIECE])
    drain(hid.at[pl.ds(0, 2 * chips - 1)], send_sem.at[HID])
    drain(ret_land.at[:, pl.ds(0, half - 1)], send_sem.at[RET])
    drain(far_land, send_sem.at[FAR])
    others = down_out.at[:, :, pl.ds(0, (tp - 1) * own_width)]
    drain(others, send_sem.at[TALL])
    drain(others, recv_sem.at[TALL])


def settle(*refs):
    copies = [
        pltpu.make_async_copy(refs[i], refs[4 + i], refs[8].at[i]) for i in (1, 2, 3, 0)
    ]
    for copy in copies:
        copy.start()
    for copy in copies:
        copy.wait()


def on_device(
    prompt, expert_ids, group_weight, expert_share, norm_gain, gate_train, up_train, down_train
):
    n = lax.axis_size("fs")
    tp = lax.axis_size("tp")
    half = n // 2
    tokens, model_width = prompt.shape
    experts_all, depth, units = gate_train.shape
    down_depth, own_width = down_train.shape[1:]
    local = experts_all // n
    hidden_width = n * down_depth
    capacity = max(2, 3 * tokens // experts_all)
    chunks = model_width // hidden_width
    width = own_width // chunks
    slots = half * 2 * capacity
    dma = pltpu.SemaphoreType.DMA
    scratch = [
        pltpu.VMEM((4, depth, units), F32),
        pltpu.VMEM((2, tokens // PROMPT_STEPS, model_width), BF16),
        pltpu.VMEM((4, n - 1, depth, units), BF16),
        pltpu.VMEM((chunks, local, hidden_width, width), BF16),
        pltpu.VMEM((2, half, local, capacity, own_width), BF16),
        pltpu.VMEM((tp, local, slots, own_width), BF16),
        pltpu.VMEM((tokens, own_width), BF16),
        pltpu.VMEM((tokens, own_width), BF16),
        pltpu.VMEM((8, tokens), F32),
        pltpu.VMEM((8, tokens), F32),
        pltpu.VMEM((depth, 128), F32),
        pltpu.VMEM((tp, local, slots, units), BF16),
        pltpu.VMEM((slots, units), F32),
        pltpu.VMEM((2, 2, half * local * capacity, tokens), BF16),
        pltpu.VMEM((2, half, local, capacity, own_width), BF16),
        pltpu.VMEM((chunks, tokens, width), BF16),
        pltpu.VMEM((chunks, tokens, width), BF16),
        pltpu.VMEM((chunks, tokens, width), F32),
        dma((4,)),
        dma((2,)),
        dma((3 * local,)),
        dma((3 * local,)),
        dma((chunks,)),
        dma((8,)),
        dma((8,)),
        dma((local,)),
        dma((local, max(1, tp // 2 - 1))),
        dma((local, tp // 2)),
        dma((local, max(1, tp // 2 - 1))),
        dma((local, tp // 2)),
        dma((max(1, local - 1),)),
        dma((chunks,)),
        dma((chunks,)),
    ]
    any_spec = pl.BlockSpec(memory_space=pl.ANY)
    vmem_spec = pl.BlockSpec(memory_space=pltpu.VMEM)
    landed = pl.pallas_call(
        functools.partial(kernel, n, tp),
        out_shape=(
            pltpu.VMEM((tokens, own_width), BF16),
            pltpu.VMEM((local, n * depth, units), BF16),
            pltpu.VMEM((local, n * depth, units), BF16),
            pltpu.VMEM((local, units, model_width), BF16),
        ),
        in_specs=[any_spec] + [vmem_spec] * 4 + [any_spec] * 3,
        out_specs=(vmem_spec,) * 4,
        scratch_shapes=scratch,
        compiler_params=pltpu.CompilerParams(
            collective_id=0, has_side_effects=True, vmem_limit_bytes=49 << 20
        ),
    )(
        prompt,
        expert_ids.T,
        group_weight[None, :],
        expert_share.T,
        norm_gain[None, :],
        gate_train,
        up_train,
        down_train,
    )
    return pl.pallas_call(
        settle,
        out_shape=tuple(jax.ShapeDtypeStruct(x.shape, x.dtype) for x in landed),
        in_specs=[vmem_spec] * 4,
        out_specs=(any_spec,) * 4,
        scratch_shapes=[dma((4,))],
        compiler_params=pltpu.CompilerParams(vmem_limit_bytes=1 << 20),
    )(*landed)


def solution(mesh):
    placed = (
        P("fs", None),
        P("fs", None),
        P("fs"),
        P("fs", None),
        P("fs"),
        P(None, "fs", "tp"),
        P(None, "fs", "tp"),
        P(None, "fs", "tp"),
    )
    return jax.shard_map(
        on_device,
        mesh=mesh,
        in_specs=placed,
        out_specs=(P("fs", "tp"), P("fs", None, "tp"), P("fs", None, "tp"), P("fs", "tp", None)),
        check_vma=False,
    )
```

```python
import functools

import jax
import jax.numpy as jnp
from jax import lax
from jax.experimental import pallas as pl
from jax.experimental.pallas import tpu as pltpu
from jax.sharding import PartitionSpec as P

EPS = 1e-06
MESH = pl.DeviceIdType.MESH
BF16 = jnp.bfloat16
F32 = jnp.float32
PROMPT_STEPS = 4
AHEAD = 2


def kernel(
    n,
    tp,
    prompt,
    ids,
    group,
    share,
    gain,
    gate_hbm,
    up_hbm,
    down_hbm,
    mixed_out,
    gate_land,
    up_land,
    down_out,
    wide,
    tall,
    sends,
    down_land,
    rows_stage,
    piece,
    own_cols,
    far_cols,
    facts,
    far_facts,
    gain_cols,
    hid,
    gate_acc,
    spread,
    ret_land,
    far_stage,
    far_land,
    total,
    load_sem,
    tall_sem,
    phase_send,
    phase_recv,
    down_recv,
    send_sem,
    recv_sem,
    rows_recv,
    chip_recv,
    mate_recv,
    hid_chip_recv,
    hid_mate_recv,
    ret_recv,
    last_ret_recv,
    far_recv,
):
    here = lax.axis_index("fs")
    me = lax.axis_index("tp")
    half = n // 2
    side = here // half
    seat = here % half
    partner = (here + half) % n
    mate = me + 1 - 2 * (me % 2)
    chips = tp // 2
    tokens, model_width = prompt.shape
    experts_all, depth, units = gate_hbm.shape
    local = experts_all // n
    last = local - 1
    capacity = ret_land.shape[3]
    own_width = own_cols.shape[1]
    down_depth = down_hbm.shape[1]
    chunks, width = down_land.shape[0], down_land.shape[3]
    seat_slots = local * capacity
    slots_of_seat = 2 * capacity
    buffers, slots_sent = wide.shape[0], sends.shape[0]
    FACTS, COLS, ROWS, PIECE, HID, RET, FAR, TALL = range(8)

    def remote(src, dst, ssem, rsem, fs=None, tp_to=None):
        device = {"fs": here if fs is None else fs, "tp": me if tp_to is None else tp_to}
        return pltpu.make_async_remote_copy(
            src_ref=src,
            dst_ref=dst,
            send_sem=ssem,
            recv_sem=rsem,
            device_id=device,
            device_id_type=MESH,
        )

    def drain(ref, sem):
        pltpu.make_async_copy(ref, ref, sem).wait()

    def at(start, size, step=16):
        return pl.ds(pl.multiple_of(start, step), size)

    def shift_of(k):
        return half + (k + 1) // 2 * (1 - 2 * (k % 2))

    def owner_of(k):
        return lax.rem(here + jnp.where(k == n - 1, 0, shift_of(k)), n)

    barrier = pltpu.get_barrier_semaphore()

    @pl.loop(1, n)
    def _(s):
        pl.semaphore_signal(
            barrier, inc=1, device_id={"fs": lax.rem(here + s, n), "tp": me}, device_id_type=MESH
        )

    @pl.loop(1, tp)
    def _(s):
        pl.semaphore_signal(
            barrier, inc=1, device_id={"fs": here, "tp": lax.rem(me + s, tp)}, device_id_type=MESH
        )

    def phase_of(e, kind):
        return 3 * e + kind

    def loads(e, kind, k):
        row = owner_of(k) * local + e
        slot = k % buffers
        if kind < 2:
            source = (gate_hbm, up_hbm)[kind]
            return [pltpu.make_async_copy(source.at[row], wide.at[slot], load_sem.at[slot])]
        return [
            pltpu.make_async_copy(
                down_hbm.at[row, :, pl.ds(c * width, width)],
                wide.at[slot, pl.ds(c * down_depth, down_depth), :],
                load_sem.at[slot],
            )
            for c in range(chunks)
        ]

    def start_loads(e, kind, k):
        for copy in loads(e, kind, k):
            copy.start()

    def wait_loads(k):
        drain(wide.at[k % buffers], load_sem.at[k % buffers])

    def cast(slot, kind):
        if kind == 2:
            return [(pl.ds(0, units), wide[slot].astype(BF16))]
        return [
            (
                pl.ds(j * 128, 128),
                (wide[slot, :, pl.ds(j * 128, 128)] * gain_cols[...]).astype(BF16),
            )
            for j in range(units // 128)
        ]

    def cast_step(e, kind, k):
        wait_loads(k)
        p = phase_of(e, kind) % slots_sent
        for cols, value in cast(k % buffers, kind):
            sends[p, k, :, cols] = value

        @pl.when(k + buffers < n)
        def _():
            start_loads(e, kind, k + buffers)

    def send_matrix(e, kind, k):
        p = phase_of(e, kind)
        land = (gate_land, up_land)[kind]
        remote(
            sends.at[p % slots_sent, k],
            land.at[e, at(here * depth, depth), :],
            phase_send.at[p],
            phase_recv.at[p],
            fs=owner_of(k),
        ).start()

    def send_down(e, c):
        p = phase_of(e, 2)

        @pl.loop(0, n - 1)
        def _(k):
            remote(
                sends.at[p % slots_sent, k, at(c * down_depth, down_depth), :],
                down_land.at[c, e, at(here * down_depth, down_depth), :],
                phase_send.at[p],
                down_recv.at[c] if e == last else phase_recv.at[p],
                fs=owner_of(k),
            ).start()

    def free_slot(p):
        if p >= slots_sent:
            drain(sends.at[p % slots_sent], phase_send.at[p - slots_sent])

    def own_block(e, kind):
        k = n - 1
        wait_loads(k)
        if kind < 2:
            land = (gate_land, up_land)[kind]
            for cols, value in cast(k % buffers, kind):
                land[e, at(here * depth, depth), cols] = value
            return
        for c in range(chunks):
            down_land[c, e, at(here * down_depth, down_depth), :] = wide[
                k % buffers, pl.ds(c * down_depth, down_depth), :
            ].astype(BF16)

    def begin(e, kind):
        for k in range(min(buffers, n)):
            start_loads(e, kind, k)

    def hand_over(e, kind, first=0):
        if not first:
            free_slot(phase_of(e, kind))
            begin(e, kind)

        @pl.loop(first, n - 1)
        def _(k):
            cast_step(e, kind, k)
            if kind < 2:

                @pl.when(k > first)
                def _():
                    send_matrix(e, kind, k - 1)

        if kind < 2:
            send_matrix(e, kind, n - 2)
        else:
            for c in range(min(AHEAD, chunks) if e == last else chunks):
                send_down(e, c)
        own_block(e, kind)

    block_rows = tokens // PROMPT_STEPS

    def load_prompt(i):
        return pltpu.make_async_copy(
            prompt.at[pl.ds(i * block_rows, block_rows)], tall.at[i % 2], tall_sem.at[i % 2]
        )

    begin(0, 0)
    load_prompt(0).start()
    load_prompt(1).start()
    gain_cols[...] = jnp.transpose(jnp.broadcast_to(gain[...], (128, depth)))

    for k in range(2):
        cast_step(0, 0, k)
    pl.semaphore_wait(barrier, n - 1 + tp - 1)
    for k in range(2):
        send_matrix(0, 0, k)

    experts = lax.broadcasted_iota(jnp.int32, (experts_all, tokens), 0)
    named = [experts == ids[pl.ds(k, 1), :] for k in range(2)]
    count = sum(m.astype(F32) for m in named).astype(BF16)
    earlier = (
        lax.broadcasted_iota(jnp.int32, (tokens, tokens), 0)
        < lax.broadcasted_iota(jnp.int32, (tokens, tokens), 1)
    ).astype(F32).astype(BF16)
    ranks = jnp.dot(count, earlier, preferred_element_type=F32)
    shares = [share[pl.ds(k, 1), :] for k in range(2)]
    facts[...] = jnp.zeros_like(facts)
    for k in range(2):
        rank = jnp.sum(jnp.where(named[k], ranks, 0.0), axis=0, keepdims=True)
        facts[pl.ds(k, 1), :] = ids[pl.ds(k, 1), :].astype(F32) * capacity + rank
        facts[pl.ds(2 + k, 1), :] = group[...] * shares[k] / (shares[0] + shares[1])

    @pl.loop(0, PROMPT_STEPS)
    def _(i):
        load_prompt(i).wait()
        squares = jnp.zeros((block_rows, 128), F32)
        for j in range(model_width // 128):
            x = tall[i % 2, :, pl.ds(j * 128, 128)].astype(F32)
            squares += x * x
        mean = jnp.sum(squares, axis=1, keepdims=True) / model_width
        scale = lax.rsqrt(mean + EPS)
        own_cols[at(i * block_rows, block_rows), :] = (
            tall[i % 2, :, at(me * own_width, own_width, 128)].astype(F32) * scale
        ).astype(BF16)

        @pl.when(i + 2 < PROMPT_STEPS)
        def _():
            load_prompt(i + 2).start()

    send_facts = remote(facts, far_facts, send_sem.at[FACTS], recv_sem.at[FACTS], fs=partner)
    send_cols = remote(own_cols, far_cols, send_sem.at[COLS], recv_sem.at[COLS], fs=partner)
    send_facts.start()
    send_cols.start()

    hand_over(0, 0, 2)

    def send_rows(q, j, e):
        to = lax.rem(seat + j, half)
        remote(
            rows_stage.at[q, to, e],
            piece.at[me, e, at((seat * 2 + q) * capacity, capacity), :],
            send_sem.at[ROWS],
            rows_recv.at[e],
            fs=side * half + to,
        ).start()

    def place_rows(q, block_facts, columns):
        targets = [block_facts[pl.ds(k, 1), :].astype(jnp.int32) for k in range(2)]

        @pl.loop(0, half)
        def _(j):
            to = lax.rem(seat + j, half)
            slots = (side * half + to) * seat_slots + lax.broadcasted_iota(
                jnp.int32, (seat_slots, tokens), 0
            )
            picker = ((slots == targets[0]) | (slots == targets[1])).astype(F32).astype(BF16)
            rows = jnp.dot(picker, columns[...], preferred_element_type=F32)
            rows_stage[q, to] = rows.astype(BF16).reshape(local, capacity, own_width)

            @pl.when(j == 0)
            def _():
                piece[me, :, at((seat * 2 + q) * capacity, capacity), :] = rows_stage[q, seat]

        for e in range(local):

            @pl.loop(1, half)
            def _(j):
                send_rows(q, j, e)

    place_rows(0, facts, own_cols)
    hand_over(0, 1)
    send_facts.wait_recv()
    send_cols.wait_recv()
    place_rows(1, far_facts, far_cols)

    hand_over(0, 2)

    def spread_tp(buffer, e, which, chip_sems, mate_sems):
        mine = buffer.at[me, e]

        @pl.loop(1, chips)
        def _(j):
            remote(
                mine,
                mine,
                send_sem.at[which],
                chip_sems.at[e, j - 1],
                tp_to=lax.rem(me + 2 * j, tp),
            ).start()

        remote(mine, mine, send_sem.at[which], mate_sems.at[e, 0], tp_to=mate).start()

    def forward_tp(buffer, e, which, chip_sems, mate_sems):
        @pl.loop(1, chips)
        def _(j):
            theirs = buffer.at[lax.rem(me + tp - 2 * j, tp), e]
            drain(theirs, chip_sems.at[e, j - 1])
            remote(theirs, theirs, send_sem.at[which], mate_sems.at[e, j], tp_to=mate).start()

    def collect_tp(buffer, e, mate_sems):
        @pl.loop(0, chips)
        def _(j):
            drain(buffer.at[0, e], mate_sems.at[e, j])

    for e in range(local):
        drain(piece.at[me, e, pl.ds(0, (half - 1) * slots_of_seat), :], rows_recv.at[e])
        spread_tp(piece, e, PIECE, chip_recv, mate_recv)

    if local > 1:
        hand_over(1, 0)
        hand_over(1, 1)

    @pl.loop(0, half)
    def _(j):
        for q in range(2):
            source = (facts, far_facts)[q]
            slots = (side * half + j) * seat_slots + lax.broadcasted_iota(
                jnp.int32, (seat_slots, tokens), 0
            )
            value = sum(
                jnp.where(
                    slots == source[pl.ds(k, 1), :].astype(jnp.int32),
                    source[pl.ds(2 + k, 1), :],
                    0.0,
                )
                for k in range(2)
            )
            high = value.astype(BF16)
            spread[q, 0, at(j * seat_slots, seat_slots), :] = high
            spread[q, 1, at(j * seat_slots, seat_slots), :] = (value - high.astype(F32)).astype(
                BF16
            )

    drain(rows_stage.at[:, pl.ds(0, half - 1)], send_sem.at[ROWS])

    def contracted(land, e):
        acc = None
        for t in range(tp):
            part = jnp.dot(
                piece[t, e],
                land[e, pl.ds(t * own_width, own_width), :],
                preferred_element_type=F32,
            )
            acc = part if acc is None else acc + part
        return acc

    def hidden(e):
        forward_tp(piece, e, PIECE, chip_recv, mate_recv)
        drain(gate_land.at[e, pl.ds(0, (n - 1) * depth), :], phase_recv.at[phase_of(e, 0)])
        collect_tp(piece, e, mate_recv)
        gate_acc[...] = contracted(gate_land, e)
        drain(up_land.at[e, pl.ds(0, (n - 1) * depth), :], phase_recv.at[phase_of(e, 1)])
        up_val = contracted(up_land, e)
        g = gate_acc[...]
        hid[me, e] = (g / (1.0 + jnp.exp(-g)) * up_val).astype(BF16)
        spread_tp(hid, e, HID, hid_chip_recv, hid_mate_recv)
        forward_tp(hid, e, HID, hid_chip_recv, hid_mate_recv)
        collect_tp(hid, e, hid_mate_recv)

    def down_cols(c, e, t):
        return down_out.at[e, :, at(t * own_width + c * width, width, 128)]

    def expert_out(c, e):
        acc = None
        for t in range(tp):
            part = jnp.dot(
                hid[t, e],
                down_land[c, e, pl.ds(t * units, units), :],
                preferred_element_type=F32,
            )
            acc = part if acc is None else acc + part
        out = acc.astype(BF16).reshape(half, 2, capacity, width)
        for m in range(half):
            for q in range(2):
                rows_stage[q, m, e, :, at(c * width, width, 128)] = out[m, q]

    def turn_down(c, e):
        down_out[e, :, at(me * own_width + c * width, width, 128)] = down_land[
            c, e, at(me * units, units), :
        ]

        @pl.loop(1, tp)
        def _(j):
            to = lax.rem(me + j, tp)
            remote(
                down_land.at[c, e, at(to * units, units), :],
                down_cols(c, e, me),
                send_sem.at[TALL],
                recv_sem.at[TALL],
                tp_to=to,
            ).start()

    def send_back(e, cols, rsem):
        for q in range(2):

            @pl.loop(1, half)
            def _(j):
                to = lax.rem(seat + j, half)
                remote(
                    rows_stage.at[q, to, e, :, cols],
                    ret_land.at[q, seat, e, :, cols],
                    send_sem.at[RET],
                    rsem,
                    fs=side * half + to,
                ).start()

        for q in range(2):
            ret_land[q, seat, e, :, cols] = rows_stage[q, seat, e, :, cols]

    for e in range(last):
        hidden(e)
        p = phase_of(e, 2)
        drain(down_land.at[:, e, pl.ds(0, (n - 1) * down_depth), :], phase_recv.at[p])

        @pl.loop(0, chunks)
        def _(c):
            expert_out(c, e)

        send_back(e, pl.ds(0, own_width), ret_recv.at[e])
        hand_over(e + 1, 2)

        @pl.loop(0, chunks)
        def _(c):
            turn_down(c, e)

        if e + 2 < local:
            hand_over(e + 2, 0)
            hand_over(e + 2, 1)

    hidden(last)
    for e in range(last):
        drain(ret_land.at[:, pl.ds(0, half - 1), e], ret_recv.at[e])

    def combine(c):
        cols = at(c * width, width, 128)
        drain(ret_land.at[:, pl.ds(0, half - 1), last, :, cols], last_ret_recv.at[c])
        for q in range(2):
            back = ret_land[q, :, :, :, cols].reshape(half * seat_slots, width)
            value = sum(
                lax.dot_general(
                    spread[q, p], back, (((0,), (0,)), ((), ())), preferred_element_type=F32
                )
                for p in range(2)
            )
            if q:
                far_stage[c] = value.astype(BF16)
            else:
                total[c] = value

    def send_far(c):
        remote(
            far_stage.at[c], far_land.at[c], send_sem.at[FAR], far_recv.at[c], fs=partner
        ).start()

    @pl.loop(0, chunks)
    def _(c):
        drain(down_land.at[c, last, pl.ds(0, (n - 1) * down_depth), :], down_recv.at[c])
        expert_out(c, last)
        send_back(last, at(c * width, width, 128), last_ret_recv.at[c])

        @pl.when(c + AHEAD < chunks)
        def _():
            send_down(last, c + AHEAD)

        turn_down(c, last)

        @pl.when(c > 0)
        def _():
            combine(c - 1)
            send_far(c - 1)

    combine(chunks - 1)
    send_far(chunks - 1)

    @pl.loop(0, chunks)
    def _(c):
        drain(far_land.at[c], far_recv.at[c])
        mixed_out[:, at(c * width, width, 128)] = (
            total[c] + far_land[c].astype(F32)
        ).astype(BF16)

    for p in range(max(0, 3 * local - slots_sent), 3 * local):
        drain(sends.at[p % slots_sent], phase_send.at[p])
    send_facts.wait_send()
    send_cols.wait_send()
    drain(piece.at[pl.ds(0, 2 * chips - 1)], send_sem.at[PIECE])
    drain(hid.at[pl.ds(0, 2 * chips - 1)], send_sem.at[HID])
    drain(ret_land.at[:, pl.ds(0, half - 1)], send_sem.at[RET])
    drain(far_land, send_sem.at[FAR])
    others = down_out.at[:, :, pl.ds(0, (tp - 1) * own_width)]
    drain(others, send_sem.at[TALL])
    drain(others, recv_sem.at[TALL])


def settle(*refs):
    copies = [
        pltpu.make_async_copy(refs[i], refs[4 + i], refs[8].at[i]) for i in (1, 2, 3, 0)
    ]
    for copy in copies:
        copy.start()
    for copy in copies:
        copy.wait()


def on_device(
    prompt, expert_ids, group_weight, expert_share, norm_gain, gate_train, up_train, down_train
):
    n = lax.axis_size("fs")
    tp = lax.axis_size("tp")
    half = n // 2
    tokens, model_width = prompt.shape
    experts_all, depth, units = gate_train.shape
    down_depth, own_width = down_train.shape[1:]
    local = experts_all // n
    hidden_width = n * down_depth
    capacity = max(2, 3 * tokens // experts_all)
    chunks = model_width // hidden_width
    width = own_width // chunks
    slots = half * 2 * capacity
    dma = pltpu.SemaphoreType.DMA
    scratch = [
        pltpu.VMEM((4, depth, units), F32),
        pltpu.VMEM((2, tokens // PROMPT_STEPS, model_width), BF16),
        pltpu.VMEM((4, n - 1, depth, units), BF16),
        pltpu.VMEM((chunks, local, hidden_width, width), BF16),
        pltpu.VMEM((2, half, local, capacity, own_width), BF16),
        pltpu.VMEM((tp, local, slots, own_width), BF16),
        pltpu.VMEM((tokens, own_width), BF16),
        pltpu.VMEM((tokens, own_width), BF16),
        pltpu.VMEM((8, tokens), F32),
        pltpu.VMEM((8, tokens), F32),
        pltpu.VMEM((depth, 128), F32),
        pltpu.VMEM((tp, local, slots, units), BF16),
        pltpu.VMEM((slots, units), F32),
        pltpu.VMEM((2, 2, half * local * capacity, tokens), BF16),
        pltpu.VMEM((2, half, local, capacity, own_width), BF16),
        pltpu.VMEM((chunks, tokens, width), BF16),
        pltpu.VMEM((chunks, tokens, width), BF16),
        pltpu.VMEM((chunks, tokens, width), F32),
        dma((4,)),
        dma((2,)),
        dma((3 * local,)),
        dma((3 * local,)),
        dma((chunks,)),
        dma((8,)),
        dma((8,)),
        dma((local,)),
        dma((local, max(1, tp // 2 - 1))),
        dma((local, tp // 2)),
        dma((local, max(1, tp // 2 - 1))),
        dma((local, tp // 2)),
        dma((max(1, local - 1),)),
        dma((chunks,)),
        dma((chunks,)),
    ]
    any_spec = pl.BlockSpec(memory_space=pl.ANY)
    vmem_spec = pl.BlockSpec(memory_space=pltpu.VMEM)
    landed = pl.pallas_call(
        functools.partial(kernel, n, tp),
        out_shape=(
            pltpu.VMEM((tokens, own_width), BF16),
            pltpu.VMEM((local, n * depth, units), BF16),
            pltpu.VMEM((local, n * depth, units), BF16),
            pltpu.VMEM((local, units, model_width), BF16),
        ),
        in_specs=[any_spec] + [vmem_spec] * 4 + [any_spec] * 3,
        out_specs=(vmem_spec,) * 4,
        scratch_shapes=scratch,
        compiler_params=pltpu.CompilerParams(
            collective_id=0, has_side_effects=True, vmem_limit_bytes=49 << 20
        ),
    )(
        prompt,
        expert_ids.T,
        group_weight[None, :],
        expert_share.T,
        norm_gain[None, :],
        gate_train,
        up_train,
        down_train,
    )
    return pl.pallas_call(
        settle,
        out_shape=tuple(jax.ShapeDtypeStruct(x.shape, x.dtype) for x in landed),
        in_specs=[vmem_spec] * 4,
        out_specs=(any_spec,) * 4,
        scratch_shapes=[dma((4,))],
        compiler_params=pltpu.CompilerParams(vmem_limit_bytes=1 << 20),
    )(*landed)


def solution(mesh):
    placed = (
        P("fs", None),
        P("fs", None),
        P("fs"),
        P("fs", None),
        P("fs"),
        P(None, "fs", "tp"),
        P(None, "fs", "tp"),
        P(None, "fs", "tp"),
    )
    return jax.shard_map(
        on_device,
        mesh=mesh,
        in_specs=placed,
        out_specs=(P("fs", "tp"), P("fs", None, "tp"), P("fs", None, "tp"), P("fs", "tp", None)),
        check_vma=False,
    )
```
